32 devices in a mesh: sp: 8 (over z, y), tp: 4 (over x, core).
Axes of the slice: x: 2, y: 2, z: 4, core: 2. Of those that a mesh axis runs over, the one named last changes fastest.
Arguments:
- tokens: bfloat16 [256, 48, 1024], P('sp', 'tp'), may hold values from -6 to 6
- norm_gain: float32 [1024], replicated, may hold values from 0.1 to 1.9
- x_weight: bfloat16 [1024, 1024], P(('sp', 'tp')), may hold values from -0.1875 to 0.1875
- gate_weight: bfloat16 [1024, 1024], P(('sp', 'tp')), may hold values from -0.1875 to 0.1875
- conv_taps: float32 [4, 1024], replicated, may hold values from -3 to 3
- rate_map: bfloat16 [2, 1024, 128], P(None, ('sp', 'tp')), may hold values from -0.5 to 0.5
- input_map: bfloat16 [2, 1024, 128], P(None, ('sp', 'tp')), may hold values from -0.5 to 0.5
- decay_rate: float32 [2, 1024], replicated, may hold values from 0.1 to 3
- out_weight: bfloat16 [1024, 1024], P(None, ('sp', 'tp')), may hold values from -0.5 to 0.5
Outputs:
- mixed_out: bfloat16 [256, 48, 1024], P('sp', 'tp')
The draws below stay inside these ranges and needn't reach their ends.
All inputs are finite; a program needn't handle non-finite values.
Results may differ from the reference program's by a relative error of at most 0.004.
Values may be sent and summed in bfloat16 or wider, within the bound.
A program may use at most 128 MiB of HBM per device.

```python
import math
import jax
import jax.numpy as jnp
from jax import lax

D = 1024
RNN_WIDTH = 1024
CONV_W = 4
SEQS = 48
RNN_BLOCK = 128
SEQ_LEN = 256


def block_scale(key, extent, pieces, low, top_value):
    gain = 1.0
    for axis_at, blocks in pieces:
        draws = jax.random.uniform(jax.random.fold_in(jax.random.fold_in(key, 6), axis_at), (blocks,), jnp.float32, low / len(pieces), top_value / len(pieces))
        gain = gain * jnp.repeat(jnp.exp(draws), extent[axis_at] // blocks).reshape((-1,) + (1,) * (len(extent) - 1 - axis_at))
    return gain


def gaussian(rng, dims, width, most, cuts=(), dtype=jnp.bfloat16):
    factor_of = block_scale(rng, dims, cuts, -0.22, 0.18) if cuts else 1.0
    values = jax.random.normal(rng, dims, jnp.float32) * width * factor_of
    return jnp.minimum(jnp.maximum(values, -most), most).astype(dtype)


def setup_inputs(seed: int = 0) -> dict:
    key_list = jax.random.split(jax.random.key(seed), 10)
    return {
        "tokens": gaussian(key_list[0], (SEQ_LEN, SEQS, D), 1.0, 6.0, ((0, 8), (1, 4))),
        "norm_gain": jnp.clip(1.0 + 0.18 * jax.random.normal(key_list[1], (D,), jnp.float32), 0.1, 1.9),
        "x_weight": gaussian(key_list[2], (D, RNN_WIDTH), D ** -0.5, 0.1875, ((0, 32),)),
        "gate_weight": gaussian(key_list[3], (D, RNN_WIDTH), D ** -0.5, 0.1875, ((0, 32),)),
        "conv_taps": gaussian(key_list[4], (CONV_W, RNN_WIDTH), CONV_W ** -0.5, 3.0, (), jnp.float32),
        "rate_map": gaussian(key_list[5], (2, RNN_WIDTH, RNN_BLOCK), RNN_BLOCK ** -0.5, 0.5, ((1, 32),)),
        "input_map": gaussian(key_list[6], (2, RNN_WIDTH, RNN_BLOCK), RNN_BLOCK ** -0.5, 0.5, ((1, 32),)),
        "decay_rate": jnp.clip(jnp.exp(jax.random.uniform(key_list[7], (2, RNN_WIDTH), jnp.float32, math.log(0.1), math.log(3.0))), 0.1, 3.0),
        "out_weight": gaussian(key_list[8], (RNN_WIDTH, D), (RNN_WIDTH // 8) ** -0.5, 0.5, ((1, 32),)),
    }


epsilon = 1e-06

def recur(conv_block, rate_block, input_block, speed, reverse):
    conv_f = conv_block.astype(jnp.float32)
    rate_gate = jax.nn.sigmoid(jnp.einsum('tsc,cd->tsd', conv_f, rate_block.astype(jnp.float32)))
    input_gate = jax.nn.sigmoid(jnp.einsum('tsc,cd->tsd', conv_f, input_block.astype(jnp.float32)))
    log_decay = -2.0 * rate_gate * speed / SEQ_LEN
    decay = jnp.exp(log_decay)
    drive = jnp.sqrt(-jnp.expm1(2.0 * log_decay)) * input_gate * conv_f

    def advance(state, inputs):
        step_decay, step_drive = inputs
        state = step_decay * state + step_drive
        return (state, state)
    initial = jnp.zeros(conv_block.shape[1:], jnp.float32)
    _, states = lax.scan(advance, initial, (decay, drive), reverse=reverse)
    return states

def reference(tokens, norm_gain, x_weight, gate_weight, conv_taps, rate_map, input_map, decay_rate, out_weight):
    length, seqs, width_in = tokens.shape
    flt = tokens.astype(jnp.float32)
    scale = lax.rsqrt(lax.optimization_barrier(jnp.mean(flt * flt, axis=-1, keepdims=True)) + epsilon)
    normed = (flt * scale * norm_gain).astype(jnp.bfloat16)
    flat = normed.reshape(length * seqs, width_in)
    channels = x_weight.shape[1]
    branch = jnp.dot(flat, x_weight, preferred_element_type=jnp.float32).astype(jnp.bfloat16).reshape(length, seqs, channels)
    gate_in = jnp.dot(flat, gate_weight, preferred_element_type=jnp.float32).astype(jnp.bfloat16).reshape(length, seqs, channels)
    padded = jnp.pad(branch, ((2, 1), (0, 0), (0, 0))).astype(jnp.float32)
    conv = padded[0:length] * conv_taps[0]
    for offset in range(1, 4):
        conv = conv + padded[offset:offset + length] * conv_taps[offset]
    conv_bf = lax.optimization_barrier(conv.astype(jnp.bfloat16))
    block_width = rate_map.shape[2]
    nblk = channels // block_width
    rate_blocks = rate_map.reshape(2, nblk, block_width, block_width)
    input_blocks = input_map.reshape(2, nblk, block_width, block_width)
    blocked = conv_bf.reshape(length, seqs, nblk, -1).transpose(2, 0, 1, 3)

    def per_block(inputs):
        conv_block, rate_fwd, rate_bwd, input_fwd, input_bwd, speed_fwd, speed_bwd = inputs
        forward = recur(conv_block, rate_fwd, input_fwd, speed_fwd, False)
        backward = recur(conv_block, rate_bwd, input_bwd, speed_bwd, True)
        return (forward + backward).astype(jnp.bfloat16)
    recurrent = lax.map(per_block, (blocked, rate_blocks[0], rate_blocks[1], input_blocks[0], input_blocks[1], decay_rate[0].reshape(nblk, -1), decay_rate[1].reshape(nblk, -1)))
    recurrent = recurrent.transpose(1, 2, 0, 3).reshape(length, seqs, channels)
    recurrent = lax.optimization_barrier(recurrent)
    gated = (recurrent.astype(jnp.float32) * jax.nn.gelu(gate_in.astype(jnp.float32))).astype(jnp.bfloat16)
    result = jnp.dot(gated.reshape(length * seqs, channels), out_weight, preferred_element_type=jnp.float32)
    return result.astype(jnp.bfloat16).reshape(length, seqs, width_in)
```

```python
import functools

import jax
import jax.numpy as jnp
from jax import lax
from jax.experimental import pallas as pl
from jax.experimental.pallas import tpu as pltpu
from jax.sharding import PartitionSpec as P

epsilon = 1e-06
MESH = pl.DeviceIdType.MESH
f32, bf16 = jnp.float32, jnp.bfloat16
ROWS = 64
COLS = 256


class Gather:
    def __init__(self, grid, place, order, own, buf, send, recv, local):
        self.grid, self.place, self.order = grid, place, order
        self.own, self.buf, self.send, self.recv, self.local = own, buf, send, recv, local
        self.copies, self.base = {}, 0
        self.bases = []
        count = 0
        for axis in order:
            self.bases.append(count)
            count += grid[axis] - 1

    def slab(self, done):
        return self.buf.at[
            tuple(
                pl.ds(0, self.grid[a]) if a in done else pl.ds(self.place[a], 1) for a in range(4)
            )
        ]

    def start(self, phase):
        axis = self.order[phase]
        made = []
        if phase == 0:
            self.kept = pltpu.make_async_copy(
                self.own, self.buf.at[tuple(self.place)], self.local
            )
            self.kept.start()
        for o in range(1, self.grid[axis]):
            there = list(self.place)
            there[axis] = lax.rem(self.place[axis] + o, self.grid[axis])
            if phase == 0:
                src, dst = self.own, self.buf.at[tuple(self.place)]
            else:
                src = dst = self.slab(self.order[:phase])
            at = self.bases[phase] + o - 1
            made.append(
                pltpu.make_async_remote_copy(
                    src_ref=src,
                    dst_ref=dst,
                    send_sem=self.send.at[at],
                    recv_sem=self.recv.at[at],
                    device_id=device(self.grid, there),
                    device_id_type=MESH,
                )
            )
            made[-1].start()
        self.copies[phase] = made

    def wait(self, phase):
        if phase == 0:
            self.kept.wait()
        for copy in self.copies[phase]:
            copy.wait_recv()

    def drain(self):
        for made in self.copies.values():
            for copy in made:
                copy.wait_send()


def device(grid, place):
    return (place[0] * grid[1] + place[1], place[2] * grid[3] + place[3])


def kernel(
    grid, gathered, seq_total, names, tok, gain, taps, speed, x_w, maps, g_w, o_w, out, *scratch
):
    r = dict(zip(names, scratch))
    n_sp = grid[0] * grid[1]
    sp, tp = lax.axis_index("sp"), lax.axis_index("tp")
    z, y = sp // grid[1], lax.rem(sp, grid[1])
    x, c = tp // grid[3], lax.rem(tp, grid[3])
    place = [z, y, x, c]
    steps, seqs, channels = r["rec"].shape
    width = tok.shape[1]
    total_rows = tok.shape[0]
    nblk, bw = r["mb"].shape[0] if gathered else maps.shape[0], 128

    barrier = pltpu.get_barrier_semaphore()
    greeted = 0
    for axis in range(4):
        if axis >= 2 and not gathered:
            continue
        for o in range(1, grid[axis]):
            there = list(place)
            there[axis] = lax.rem(place[axis] + o, grid[axis])
            pl.semaphore_signal(
                barrier, inc=1, device_id=device(grid, there), device_id_type=MESH
            )
            greeted += 1
    before, after = lax.rem(sp + n_sp - 1, n_sp), lax.rem(sp + 1, n_sp)
    for there in (before, after):
        pl.semaphore_signal(barrier, inc=1, device_id=(there, tp), device_id_type=MESH)
        greeted += 1
    pl.semaphore_wait(barrier, greeted)

    if gathered:
        outward, inward = (2, 1, 0, 3), (0, 1, 2, 3)
        gx, gm, gg, go = (
            Gather(grid, place, order, own, r[name], r["send"].at[i], r["recv"].at[i], r["local"].at[i])
            for i, (name, order, own) in enumerate(
                (("wx", outward, x_w), ("wm", inward, maps), ("wg", inward, g_w), ("wo", outward, o_w))
            )
        )
        gx.start(0)
        gm.start(0)
        gg.start(0)

    def advance(g, phase):
        if gathered:
            g.wait(phase)
            if phase < 3:
                g.start(phase + 1)

    if not gathered:
        gx = gm = gg = go = None

    def norm_rows(i, _):
        rows = pl.ds(pl.multiple_of(i * ROWS, ROWS), ROWS)
        flt = tok[rows, :].astype(f32)
        scale = lax.rsqrt(jnp.mean(flt * flt, axis=-1, keepdims=True) + epsilon)
        r["normed"][rows, :] = (flt * scale * gain[...]).astype(bf16)
        return 0

    half = total_rows // ROWS // 2
    lax.fori_loop(0, half, norm_rows, 0)
    advance(gx, 0)
    lax.fori_loop(half, total_rows // ROWS, norm_rows, 0)
    advance(gx, 1)
    advance(gm, 0)
    advance(gg, 0)
    advance(gm, 1)
    advance(gx, 2)
    if gathered:
        go.start(0)
    advance(gm, 2)
    advance(gx, 3)

    def columns_of(name, ref, at):
        if gathered:
            return r[name][:, :, :, :, :, pl.ds(at, COLS)].reshape(width, COLS)
        return ref[:, pl.ds(at, COLS)]

    def project_branch(i, _):
        at = pl.multiple_of(i * COLS, COLS)
        piece = jnp.dot(
            r["normed"][...], columns_of("wx", x_w, at), preferred_element_type=f32
        ).astype(bf16)
        r["br"][pl.ds(2, steps), :, pl.ds(at, COLS)] = piece.reshape(steps, seqs, COLS)
        return 0

    lax.fori_loop(0, channels // COLS, project_branch, 0)
    head = pltpu.make_async_remote_copy(
        src_ref=r["br"].at[pl.ds(2, 1)],
        dst_ref=r["hi"],
        send_sem=r["hsend"].at[0],
        recv_sem=r["hrecv"].at[0],
        device_id=(before, tp),
        device_id_type=MESH,
    )
    tail = pltpu.make_async_remote_copy(
        src_ref=r["br"].at[pl.ds(steps, 2)],
        dst_ref=r["lo"],
        send_sem=r["hsend"].at[1],
        recv_sem=r["hrecv"].at[1],
        device_id=(after, tp),
        device_id_type=MESH,
    )
    head.start()
    tail.start()
    advance(gm, 3)
    if gathered:
        slab_rows = maps.shape[1]
        for d in range(nblk * bw // slab_rows):
            s, t = divmod(d, grid[2] * grid[3])
            at = (s // grid[1], s % grid[1], t // grid[3], t % grid[3])
            block, low = divmod(d * slab_rows, bw)
            for k in range(4):
                r["mb"][block, low : low + slab_rows, k * bw : (k + 1) * bw] = r["wm"][at + (k,)]
    head.wait_recv()
    tail.wait_recv()
    r["br"][0:2] = jnp.where(sp > 0, r["lo"][...], jnp.zeros_like(r["lo"]))
    r["br"][steps + 2 : steps + 3] = jnp.where(
        sp < n_sp - 1, r["hi"][...], jnp.zeros_like(r["hi"])
    )
    advance(gg, 1)
    advance(go, 0)

    group = 4

    def terms(i, k, lanes):
        t = pl.ds(pl.multiple_of(i * group, group), group)
        rate = 0.5 * jnp.tanh(0.5 * r["gates"][t, :, k * bw : (k + 1) * bw]) + 0.5
        inp = 0.5 * jnp.tanh(0.5 * r["gates"][t, :, (k + 2) * bw : (k + 3) * bw]) + 0.5
        factor = (speed[k : k + 1, lanes] * (-2.0 / seq_total)).reshape(1, 1, bw)
        log_decay = rate * factor
        decay = jnp.exp(log_decay)
        u = 2.0 * log_decay
        gone = -u * (1.0 + u * (1 / 2 + u * (1 / 6 + u * (1 / 24 + u * (1 / 120)))))
        root = gone * lax.rsqrt(jnp.maximum(gone, 1e-37))
        return decay, root * inp * r["cf"][t].astype(f32)

    def block_step(b, _):
        lanes = pl.ds(pl.multiple_of(b * bw, bw), bw)

        def conv_rows(i, _):
            t0 = i * group
            conv = r["br"][pl.ds(t0, group), :, lanes].astype(f32) * taps[0:1, lanes].reshape(1, 1, bw)
            for j in range(1, 4):
                conv = conv + r["br"][pl.ds(t0 + j, group), :, lanes].astype(f32) * taps[
                    j : j + 1, lanes
                ].reshape(1, 1, bw)
            r["cf"][pl.ds(t0, group)] = conv.astype(bf16)
            return 0

        lax.fori_loop(0, steps // group, conv_rows, 0)
        mat = r["mb"][b] if gathered else maps[b]
        r["gates"][...] = jnp.dot(
            r["cf"][...].reshape(steps * seqs, bw), mat, preferred_element_type=f32
        ).reshape(steps, seqs, 4 * bw)

        def forward(i, carry):
            prod, state = carry
            decay, drive = terms(i, 0, lanes)
            for j in range(group):
                prod = prod * decay[j]
                state = state * decay[j] + drive[j]
                r["pf"][i * group + j, :, lanes] = prod
                r["rec"][i * group + j, :, lanes] = state
            return prod, state

        one, zero = jnp.ones((seqs, bw), f32), jnp.zeros((seqs, bw), f32)
        prod, state = lax.fori_loop(0, steps // group, forward, (one, zero))
        r["sum"][0, 0, :, lanes] = prod
        r["sum"][0, 1, :, lanes] = state

        def backward(i, carry):
            prod, state = carry
            i = steps // group - 1 - i
            decay, drive = terms(i, 1, lanes)
            for j in reversed(range(group)):
                prod = prod * decay[j]
                state = state * decay[j] + drive[j]
                r["pb"][i * group + j, :, lanes] = prod
                r["rec"][i * group + j, :, lanes] += state
            return prod, state

        prod, state = lax.fori_loop(0, steps // group, backward, (one, zero))
        r["sum"][1, 0, :, lanes] = prod
        r["sum"][1, 1, :, lanes] = state
        return 0

    lax.fori_loop(0, nblk // 2, block_step, 0)
    advance(gg, 2)
    advance(go, 1)
    lax.fori_loop(nblk // 2, nblk, block_step, 0)

    mates = []
    for o in range(1, grid[1]):
        there = list(place)
        there[1] = lax.rem(y + o, grid[1])
        mates.append(
            pltpu.make_async_remote_copy(
                src_ref=r["sum"],
                dst_ref=r["mate"].at[o - 1],
                send_sem=r["ysend"].at[o - 1],
                recv_sem=r["yrecv"].at[o - 1],
                device_id=device(grid, there),
                device_id_type=MESH,
            )
        )
        mates[-1].start()
    advance(gg, 3)

    def project_gate(i, _):
        at = pl.multiple_of(i * COLS, COLS)
        piece = jnp.dot(
            r["normed"][...], columns_of("wg", g_w, at), preferred_element_type=f32
        ).astype(bf16)
        r["gate"][:, pl.ds(at, COLS)] = piece
        return 0

    lax.fori_loop(0, channels // COLS // 2, project_gate, 0)
    for copy in mates:
        copy.wait_recv()
    first = y == 0
    mine = [[r["sum"][k, q] for q in range(2)] for k in range(2)]
    theirs = [[r["mate"][0, k, q] for q in range(2)] for k in range(2)]
    for k in range(2):
        mine_first = first if k == 0 else jnp.logical_not(first)
        r["pair"][k, 0] = mine[k][0] * theirs[k][0]
        r["pair"][k, 1] = jnp.where(
            mine_first,
            theirs[k][0] * mine[k][1] + theirs[k][1],
            mine[k][0] * theirs[k][1] + mine[k][1],
        )
    across = []
    for o in range(1, grid[0]):
        there = list(place)
        there[0] = lax.rem(z + o, grid[0])
        way = (z + o) // grid[0]
        across.append(
            pltpu.make_async_remote_copy(
                src_ref=r["pair"].at[way],
                dst_ref=r["far"].at[o - 1],
                send_sem=r["zsend"].at[o - 1],
                recv_sem=r["zrecv"].at[o - 1],
                device_id=device(grid, there),
                device_id_type=MESH,
            )
        )
        across[-1].start()
    lax.fori_loop(channels // COLS // 2, channels // COLS, project_gate, 0)

    advance(go, 2)
    for copy in across:
        copy.wait_recv()
    hf = jnp.zeros((seqs, channels), f32)
    for o in range(grid[0] - 1, 0, -1):
        longer = r["far"][o - 1, 0] * hf + r["far"][o - 1, 1]
        hf = jnp.where(o <= z, longer, hf)
    hf = jnp.where(first, hf, r["mate"][0, 0, 0] * hf + r["mate"][0, 0, 1])
    r["hf"][...] = hf
    hb = jnp.zeros((seqs, channels), f32)
    for o in range(1, grid[0]):
        longer = r["far"][o - 1, 0] * hb + r["far"][o - 1, 1]
        hb = jnp.where(o > z, longer, hb)
    hb = jnp.where(first, r["mate"][0, 1, 0] * hb + r["mate"][0, 1, 1], hb)
    r["hb"][...] = hb

    def finish(i, _):
        rows = pl.ds(pl.multiple_of(i * seqs, seqs), seqs)
        for low in range(0, channels, COLS):
            lanes = pl.ds(low, COLS)
            recurrent = (
                r["rec"][i, :, lanes]
                + r["pf"][i, :, lanes] * r["hf"][:, lanes]
                + r["pb"][i, :, lanes] * r["hb"][:, lanes]
            ).astype(bf16).astype(f32)
            g = r["gate"][rows, lanes].astype(f32)
            inner = 0.7978845608028654 * (g + 0.044715 * (g * g * g))
            r["gated"][rows, lanes] = (
                recurrent * (g * (0.5 * (1.0 + jnp.tanh(inner))))
            ).astype(bf16)
        return 0

    lax.fori_loop(0, steps, finish, 0)
    advance(go, 3)
    o_tiles = grid[0] if gathered else width // COLS

    def project_out(i, _):
        wide = width // o_tiles
        at = pl.multiple_of(i * wide, 128)
        if gathered:
            mat = r["wo"][pl.ds(i, 1)].reshape(wide, channels)
            dims = (((1,), (1,)), ((), ()))
        else:
            mat = o_w[:, pl.ds(at, wide)]
            dims = (((1,), (0,)), ((), ()))
        piece = lax.dot_general(r["gated"][...], mat, dims, preferred_element_type=f32)
        out[:, pl.ds(at, wide)] = piece.astype(bf16)
        return 0

    lax.fori_loop(0, o_tiles, project_out, 0)
    head.wait_send()
    tail.wait_send()
    for copy in mates + across:
        copy.wait_send()
    if gathered:
        for g in (gx, gm, gg, go):
            g.drain()


def shards(
    sizes, tokens, norm_gain, x_weight, gate_weight, conv_taps, rate_map, input_map, decay_rate, out_weight
):
    n_sp, n_tp = sizes
    grid = (n_sp // 2, 2, n_tp // 2, 2)
    steps, seqs_here, width = tokens.shape
    channels = x_weight.shape[1]
    slab = x_weight.shape[0]
    bw = rate_map.shape[2]
    nblk = channels // bw
    seqs = -(-seqs_here // 16) * 16
    gathered = slab % 16 == 0
    tok = jnp.pad(tokens, ((0, 0), (0, seqs - seqs_here), (0, 0))).reshape(steps * seqs, width)
    maps = jnp.concatenate([rate_map, input_map], axis=0)
    if gathered:
        x_w, g_w, o_w = x_weight, gate_weight, out_weight.T
    else:
        both = ("sp", "tp")
        x_w = lax.all_gather(x_weight, both, axis=0, tiled=True)
        g_w = lax.all_gather(gate_weight, both, axis=0, tiled=True)
        o_w = lax.all_gather(out_weight, both, axis=1, tiled=True)
        maps = lax.all_gather(maps, both, axis=1, tiled=True)
        maps = maps.reshape(4, nblk, bw, bw).transpose(1, 2, 0, 3).reshape(nblk, bw, 4 * bw)

    spec = {
        "normed": pltpu.VMEM((steps * seqs, width), bf16),
        "br": pltpu.VMEM((steps + 3, seqs, channels), bf16),
        "lo": pltpu.VMEM((2, seqs, channels), bf16),
        "hi": pltpu.VMEM((1, seqs, channels), bf16),
        "cf": pltpu.VMEM((steps, seqs, bw), bf16),
        "gates": pltpu.VMEM((steps, seqs, 4 * bw), f32),
        "rec": pltpu.VMEM((steps, seqs, channels), f32),
        "pf": pltpu.VMEM((steps, seqs, channels), f32),
        "pb": pltpu.VMEM((steps, seqs, channels), f32),
        "gate": pltpu.VMEM((steps * seqs, channels), bf16),
        "gated": pltpu.VMEM((steps * seqs, channels), bf16),
        "sum": pltpu.VMEM((2, 2, seqs, channels), f32),
        "pair": pltpu.VMEM((2, 2, seqs, channels), f32),
        "mate": pltpu.VMEM((grid[1] - 1, 2, 2, seqs, channels), f32),
        "far": pltpu.VMEM((grid[0] - 1, 2, seqs, channels), f32),
        "hf": pltpu.VMEM((seqs, channels), f32),
        "hb": pltpu.VMEM((seqs, channels), f32),
        "hsend": pltpu.SemaphoreType.DMA((2,)),
        "hrecv": pltpu.SemaphoreType.DMA((2,)),
        "ysend": pltpu.SemaphoreType.DMA((grid[1] - 1,)),
        "yrecv": pltpu.SemaphoreType.DMA((grid[1] - 1,)),
        "zsend": pltpu.SemaphoreType.DMA((grid[0] - 1,)),
        "zrecv": pltpu.SemaphoreType.DMA((grid[0] - 1,)),
    }
    if gathered:
        hops = sum(grid) - 4
        spec |= {
            "wx": pltpu.VMEM(grid + (slab, channels), bf16),
            "wg": pltpu.VMEM(grid + (slab, channels), bf16),
            "wo": pltpu.VMEM(grid + (slab, channels), bf16),
            "wm": pltpu.VMEM(grid + (4, slab, bw), bf16),
            "mb": pltpu.VMEM((nblk, bw, 4 * bw), bf16),
            "send": pltpu.SemaphoreType.DMA((4, hops)),
            "recv": pltpu.SemaphoreType.DMA((4, hops)),
            "local": pltpu.SemaphoreType.DMA((4,)),
        }
    out = pl.pallas_call(
        functools.partial(kernel, grid, gathered, steps * n_sp, tuple(spec)),
        out_shape=jax.ShapeDtypeStruct((steps * seqs, width), bf16),
        in_specs=[pl.BlockSpec(memory_space=pltpu.VMEM)] * 8,
        out_specs=pl.BlockSpec(memory_space=pltpu.VMEM),
        scratch_shapes=list(spec.values()),
        compiler_params=pltpu.CompilerParams(
            collective_id=0, has_side_effects=True, vmem_limit_bytes=60 * 1024 * 1024
        ),
    )(tok, norm_gain.reshape(1, width), conv_taps, decay_rate, x_w, maps, g_w, o_w)
    return out.reshape(steps, seqs, width)[:, :seqs_here]


def solution(mesh):
    placed = (
        P("sp", "tp", None),
        P(),
        P(("sp", "tp"), None),
        P(("sp", "tp"), None),
        P(),
        P(None, ("sp", "tp"), None),
        P(None, ("sp", "tp"), None),
        P(),
        P(None, ("sp", "tp")),
    )
    return jax.shard_map(
        functools.partial(shards, (mesh.shape["sp"], mesh.shape["tp"])),
        mesh=mesh,
        in_specs=placed,
        out_specs=P("sp", "tp", None),
        check_vma=False,
    )
```
